32 devices in a mesh: ep: 4 (over y, x), tp: 8 (over z, core).
Axes of the slice: x: 2, y: 2, z: 4, core: 2. Of those that a mesh axis runs over, the one named last changes fastest.
Arguments:
- query_preactivation: bfloat16 [8192, 2048], P('ep', 'tp'), may hold values from -6 to 6
- forget_preactivation: bfloat16 [8192, 2048], P('ep', 'tp'), may hold values from -6 to 6
- value_input_rows: bfloat16 [8192, 1024], P('ep', 'tp'), may hold values from -8 to 8
- output_gate_preactivation: bfloat16 [8192, 1024], P('ep', 'tp'), may hold values from -6 to 6
- forget_floor_gap: float32 [2048], P('tp'), may hold values from 0 to 0.2, as said below
- extra_log_forget: float32 [8192, 16], P('ep', 'tp'), may hold values from -2 to 0
- head_output_gain: float32 [1024], P('tp'), may hold values from 0.1 to 1.9
- mixer_output_weight: bfloat16 [1024, 2048], P(None, 'tp'), may hold values from -0.1875 to 0.1875
- second_batch_tokens: bfloat16 [2048, 2048], P('ep'), may hold values from -6 to 6
- feedforward_norm_gain: float32 [2048], replicated, may hold values from 0.1 to 1.9
- chosen_expert_index: int32 [2048, 2], P('ep'), may hold values from 0 to 3, all different within a row; in each aligned block of 64 rows (0 to 63, 64 to 127, ...) at most 40 rows name the same one
- chosen_expert_weight: float32 [2048, 2], P('ep'), may hold values from 0.1 to 1
- expert_gate_weight: bfloat16 [4, 2048, 7168], P('ep', None, 'tp'), may hold values from -0.125 to 0.125
- expert_up_weight: bfloat16 [4, 2048, 7168], P('ep', None, 'tp'), may hold values from -0.125 to 0.125
- expert_down_weight: bfloat16 [4, 7168, 2048], P('ep', 'tp'), may hold values from -0.0625 to 0.0625
Outputs:
- mixer_output_first: bfloat16 [8192, 2048], P('ep', 'tp')
- moe_out: bfloat16 [2048, 2048], P(('ep', 'tp'))
The draws below stay inside these ranges and needn't reach their ends.
Inputs may be any that keep to these rules, and one draw needn't show every extreme that they name: `chosen_expert_index`: each row names 2 different experts. In each aligned block of 64 rows (the rows of one device's share) no expert is named by more than 40 rows, and in every draw some expert is named by exactly 40 rows of some block. `forget_floor_gap`: every entry is positive.
All inputs are finite; a program needn't handle non-finite values.
Results may differ from the reference program's by a relative error of at most 0.019.
Values may be sent and summed in bfloat16 or wider, within the bound.
A program may use at most 128 MiB of HBM per device.

```python
import math
import jax
import jax.numpy as jnp
import numpy as np
from jax import lax

D = 2048
RECURRENT_HEADS = 16
KEY_DIM = 128
VAL_DIM = 64
KW = 2048
VW = 1024
BLOCK_POSITIONS = 64
SEG_A = 2048
TOKENS_A = 8192
TOKENS_B = 2048
SUB_B = 64
EXPERTS = 4
FFE = 7168
FFE_DEV = 896
TOPK = 2
CAP = 40
N_TP = 8


def draw_value_input_rows(key, part):
    noise_key, offset_key = jax.random.split(key)
    noise_part = jnp.clip(jax.random.normal(noise_key, (TOKENS_A, VW), jnp.float32), -6.0, 6.0)
    offsets = jax.random.uniform(offset_key, (1, VW), jnp.float32, -1.0, 1.0)
    return (noise_part + offsets).astype(jnp.bfloat16)


def draw_forget_floor_gap(key, part):
    choose_key, slow_key, fast_key = jax.random.split(key, 3)
    slow_share = 0.5
    chosen = jax.random.uniform(choose_key, (KW,), jnp.float32) < slow_share
    slow_rate = jnp.exp(jax.random.uniform(slow_key, (KW,), jnp.float32, jnp.log(0.05 / TOKENS_A), jnp.log(1.0 / TOKENS_A)))
    fast_rate = jnp.exp(jax.random.uniform(fast_key, (KW,), jnp.float32, jnp.log(0.06), jnp.log(0.2)))
    return jnp.where(chosen, slow_rate, fast_rate)


def draw_extra_log_forget(key, part):
    rate_key, place_key, depth_key = jax.random.split(key, 3)
    segments = TOKENS_A // SEG_A
    rates = jnp.exp(jax.random.uniform(rate_key, (segments, 1, RECURRENT_HEADS), jnp.float32, jnp.log(0.1 / TOKENS_A), jnp.log(0.4 / TOKENS_A)))
    base_log = -jnp.broadcast_to(rates, (segments, SEG_A, RECURRENT_HEADS)).reshape(TOKENS_A, RECURRENT_HEADS)
    places = jax.random.randint(place_key, (2, RECURRENT_HEADS), 0, TOKENS_A)
    depths = jax.random.uniform(depth_key, (2, RECURRENT_HEADS), jnp.float32, jnp.log(0.5), jnp.log(0.8))
    columns = jnp.broadcast_to(jnp.arange(RECURRENT_HEADS, dtype=jnp.int32)[None, :], (2, RECURRENT_HEADS))
    return base_log.at[places, columns].add(depths)


def block_scale(own_key, shape, shards, least, high):
    level, own = 1.0, jax.random.fold_in(own_key, 6)
    for axis_at, shards_of in shards:
        heights = jnp.exp(jax.random.uniform(jax.random.fold_in(own, axis_at), (shards_of,), jnp.float32, least / len(shards), high / len(shards)))
        level = level * jnp.repeat(heights, shape[axis_at] // shards_of).reshape([-1 if axis == axis_at else 1 for axis in range(len(shape))])
    return level


def assign_block(own_key, own, number, rows, count, top, limit, lean):
    ranking = jax.random.permutation(own_key, count)
    crowded, usual = portions_of(count, rows * top, limit, lean, True), portions_of(count, rows * top, limit, lean, False)
    places = jnp.arange(count)

    def named(lengths, turn):
        used = int((lengths > 0).sum())
        fixed = max(1, used // 4)
        shifted = fixed + (places - fixed + turn * (used - fixed)) % max(1, count - fixed)
        return jnp.zeros((count,), jnp.int32).at[ranking[jnp.where(places < fixed, places, shifted)]].set(jnp.asarray(lengths, jnp.int32))

    lengths = jnp.where(number % 4 == 0, named(crowded, number // 4), named(usual, number - number // 4 - 1))
    mixed = jax.random.permutation(jax.random.fold_in(own, 3), count)
    giver, receiver = mixed[0:count // 2 * 2:2], mixed[1:count // 2 * 2:2]
    room = jnp.minimum(lengths[giver] - 1, limit - lengths[receiver]) // 2
    room = jnp.where((giver == ranking[0]) | (receiver == ranking[0]) | (lengths[receiver] == 0), 0, jnp.maximum(room, 0))
    shifted = jax.random.randint(jax.random.fold_in(own, 4), (count // 2,), 0, 1 << 20) % (room + 1)
    lengths = lengths.at[giver].add(-shifted).at[receiver].add(shifted)
    labels = jnp.searchsorted(jnp.cumsum(lengths), jnp.arange(rows * top), side="right").astype(jnp.int32)
    listing = labels.reshape(top, rows).T
    listing = listing[jax.random.permutation(jax.random.fold_in(own, 1), rows)]
    turn = jax.random.randint(jax.random.fold_in(own, 2), (rows, 1), 0, top)
    return jnp.take_along_axis(listing, (jnp.arange(top)[None, :] + turn) % top, axis=1)


def portions_of(amount, total, reach, skew, full):
    portions = [(1 << 20) // math.isqrt(grade ** skew) + 1 for grade in range(1, amount + 1)]
    largest = reach if full else min(reach, max(-(-total // amount), total * portions[0] // sum(portions)))
    least = 1 if total - largest >= amount - 1 else 0
    counts, spare = [largest] + [least] * (amount - 1), total - largest - least * (amount - 1)
    while spare > 0:
        candidates = [i for i in range(1, amount) if counts[i] < largest] or [i for i in range(1, amount) if counts[i] < reach]
        pool, left = sum([portions[i] for i in candidates]), spare
        for i in candidates:
            more = min(reach - counts[i], max(1, left * portions[i] // pool), spare)
            counts[i] = counts[i] + more
            spare = spare - more
    return np.array(counts)


def scatter_about(own_key, dims, deviation, bound, cuts=(), kind=jnp.bfloat16):
    array = deviation * jax.random.normal(own_key, dims, jnp.float32)
    if cuts:
        array = array * block_scale(own_key, dims, cuts, -0.22, 0.18)
    return jnp.clip(array, -bound, bound).astype(kind)


def setup_inputs(seed: int = 0) -> dict:
    key_of = jax.random.split(jax.random.key(seed), 16)
    query_preactivation = scatter_about(key_of[0], (TOKENS_A, KW), 1.0, 6.0, ((0, 4), (1, 8)))
    forget_preactivation = scatter_about(key_of[1], (TOKENS_A, KW), 1.0, 6.0, ((0, 4), (1, 8)))
    value_input_rows = draw_value_input_rows(jax.random.fold_in(key_of[15], 71), 0)
    output_gate_preactivation = scatter_about(key_of[3], (TOKENS_A, VW), 1.0, 6.0, ((0, 4), (1, 8)))
    forget_floor_gap = draw_forget_floor_gap(jax.random.fold_in(key_of[15], 71), 0)
    extra_log_forget = draw_extra_log_forget(jax.random.fold_in(key_of[15], 71), 0)
    head_output_gain = jnp.clip(1.0 + 0.18 * jax.random.normal(key_of[6], (VW,), jnp.float32), 0.1, 1.9)
    mixer_output_weight = scatter_about(key_of[7], (VW, D), VW ** -0.5, 0.1875, ((1, 8),))
    second_batch_tokens = scatter_about(key_of[8], (TOKENS_B, D), 1.0, 6.0, ((0, 4),))
    feedforward_norm_gain = jnp.clip(1.0 + 0.18 * jax.random.normal(key_of[9], (D,), jnp.float32), 0.1, 1.9)
    chosen_expert_index_keys = jax.random.split(jax.random.fold_in(key_of[10], 1), TOKENS_B // SUB_B)
    chosen_expert_index_turns = jax.random.permutation(jax.random.fold_in(key_of[10], 3), TOKENS_B // SUB_B)
    chosen_expert_index = jax.vmap(lambda own, number: assign_block(jax.random.fold_in(key_of[10], 2), own, number, SUB_B, EXPERTS, TOPK, CAP, 1))(chosen_expert_index_keys, chosen_expert_index_turns).reshape((TOKENS_B, TOPK))
    chosen_expert_weight = jnp.clip(0.1 + 0.9 * jax.random.uniform(key_of[11], (TOKENS_B, TOPK), jnp.float32) ** block_scale(key_of[11], (TOKENS_B, TOPK), ((0, 4),), -0.2, 0.2), 0.1, 1.0)
    expert_gate_weight = scatter_about(key_of[12], (EXPERTS, D, FFE), D ** -0.5, 0.125, ((0, 4), (2, 8)))
    expert_up_weight = scatter_about(key_of[13], (EXPERTS, D, FFE), D ** -0.5, 0.125, ((0, 4), (2, 8)))
    expert_down_weight = scatter_about(key_of[14], (EXPERTS, FFE, D), FFE ** -0.5, 0.0625, ((0, 4), (1, 8)))
    return {"query_preactivation": query_preactivation, "forget_preactivation": forget_preactivation, "value_input_rows": value_input_rows, "output_gate_preactivation": output_gate_preactivation, "forget_floor_gap": forget_floor_gap, "extra_log_forget": extra_log_forget, "head_output_gain": head_output_gain, "mixer_output_weight": mixer_output_weight, "second_batch_tokens": second_batch_tokens, "feedforward_norm_gain": feedforward_norm_gain, "chosen_expert_index": chosen_expert_index, "chosen_expert_weight": chosen_expert_weight, "expert_gate_weight": expert_gate_weight, "expert_up_weight": expert_up_weight, "expert_down_weight": expert_down_weight}


highest_accuracy = lax.Precision.HIGHEST
epsilon = 1e-06

def slot_positions(blocks):
    flattened = blocks.reshape(blocks.shape[0], -1)
    onehot = (flattened[..., None] == jnp.arange(EXPERTS, dtype=jnp.int32)).astype(jnp.int32)
    earlier = jnp.cumsum(onehot, axis=1) - onehot
    return lax.optimization_barrier(jnp.sum(earlier * onehot, axis=-1)).reshape(blocks.shape)

def mixer_portion(query_preactivation, forget_preactivation, value_input_rows, output_gate_preactivation, forget_floor_gap, extra_log_forget, head_output_gain, mixer_output_weight):
    length = query_preactivation.shape[0]
    block_count = length // BLOCK_POSITIONS
    shape_key = (block_count, BLOCK_POSITIONS, RECURRENT_HEADS, KEY_DIM)
    queries = jax.nn.silu(query_preactivation.astype(jnp.float32)).reshape(shape_key)
    key_decay_rates = forget_floor_gap.reshape(RECURRENT_HEADS, KEY_DIM) * jax.nn.sigmoid(-forget_preactivation.astype(jnp.float32)).reshape(shape_key)
    forget_log_factor = jnp.log(1.0 - key_decay_rates) + extra_log_forget.reshape(block_count, BLOCK_POSITIONS, RECURRENT_HEADS)[..., None]
    values = value_input_rows.astype(jnp.float32).reshape(block_count, BLOCK_POSITIONS, RECURRENT_HEADS, VAL_DIM)
    causal_mask = jnp.arange(BLOCK_POSITIONS)[:, None] >= jnp.arange(BLOCK_POSITIONS)[None, :]

    def advance(recurrent_state_matrix, inputs):
        query_block_rows, block_key, value_block_rows, block_log = inputs
        cumulative_log = jnp.cumsum(block_log, axis=0)
        block_final_row = cumulative_log[-1]
        query_scaled = query_block_rows * jnp.exp(cumulative_log - block_final_row)
        scaled_key_rows = block_key * jnp.exp(block_final_row - cumulative_log)
        scores = jnp.einsum('thk,shk->hts', query_scaled, scaled_key_rows, precision=highest_accuracy)
        scores = jnp.where(causal_mask, scores, 0.0)
        within = jnp.einsum('hts,shv->thv', scores, value_block_rows, precision=highest_accuracy)
        across_blocks = jnp.einsum('pjy,jyr->pjr', query_block_rows * jnp.exp(cumulative_log), recurrent_state_matrix, precision=highest_accuracy)
        recurrent_state_matrix = jnp.exp(block_final_row)[..., None] * recurrent_state_matrix + jnp.einsum('jnz,jne->nze', scaled_key_rows, value_block_rows, precision=highest_accuracy)
        return (recurrent_state_matrix, within + across_blocks)
    initial = jnp.zeros((RECURRENT_HEADS, KEY_DIM, VAL_DIM), jnp.float32)
    final_state, outputs = lax.scan(advance, initial, (queries, key_decay_rates, values, forget_log_factor))
    recurrent = outputs.reshape(length, RECURRENT_HEADS, VAL_DIM)
    factor = lax.rsqrt(lax.optimization_barrier(jnp.mean(recurrent * recurrent, axis=-1, keepdims=True)) + epsilon)
    normed = (recurrent * factor * head_output_gain.reshape(RECURRENT_HEADS, VAL_DIM)).reshape(length, RECURRENT_HEADS * VAL_DIM)
    mixed = (normed * jax.nn.silu(output_gate_preactivation.astype(jnp.float32))).astype(jnp.bfloat16)
    return jnp.dot(mixed, mixer_output_weight, preferred_element_type=jnp.float32).astype(jnp.bfloat16)

def expert_part(second_batch_tokens, feedforward_norm_gain, chosen_expert_index, chosen_expert_weight, expert_gate_weight, expert_up_weight, expert_down_weight):
    total_rows = second_batch_tokens.shape[0]
    width = second_batch_tokens.shape[1]
    tokens_float = second_batch_tokens.astype(jnp.float32)
    factor = lax.rsqrt(lax.optimization_barrier(jnp.mean(tokens_float * tokens_float, axis=-1, keepdims=True)) + epsilon)
    normed = (tokens_float * factor * feedforward_norm_gain).astype(jnp.bfloat16)
    nsub = total_rows // SUB_B
    blocks = chosen_expert_index.reshape(nsub, SUB_B, TOPK)
    slot_ids = slot_positions(blocks)
    sub_index = jnp.arange(nsub, dtype=jnp.int32)[:, None, None]
    flat_slot = (blocks * nsub + sub_index) * CAP + slot_ids
    token_ids = jnp.broadcast_to(jnp.arange(total_rows, dtype=jnp.int32).reshape(nsub, SUB_B, 1), blocks.shape)
    lookup = jnp.full((EXPERTS * nsub * CAP,), -1, jnp.int32).at[flat_slot.reshape(-1)].set(token_ids.reshape(-1))
    lookup = lookup.reshape(EXPERTS, nsub * CAP)

    def one_expert(inputs):
        row_index, gate_weight, up_weight, down_weight = inputs
        picked = normed[jnp.maximum(row_index, 0)]
        routed = jnp.where((row_index >= 0)[:, None], picked, jnp.zeros((), jnp.bfloat16))
        gate_part = jnp.dot(routed, gate_weight, preferred_element_type=jnp.float32)
        up_part = jnp.dot(routed, up_weight, preferred_element_type=jnp.float32)
        hidden = (jax.nn.silu(gate_part) * up_part).astype(jnp.bfloat16)
        hidden_groups = jnp.transpose(hidden.reshape(-1, N_TP, FFE_DEV), (1, 0, 2))
        down_groups = down_weight.reshape(N_TP, FFE_DEV, width)

        def add_group(running, pair):
            product = jnp.dot(pair[0], pair[1], preferred_element_type=jnp.float32)
            return (running + lax.optimization_barrier(product.astype(jnp.bfloat16)).astype(jnp.float32), None)
        running, unused = lax.scan(add_group, jnp.zeros((hidden.shape[0], width), jnp.float32), (hidden_groups, down_groups))
        return running.astype(jnp.bfloat16)
    outputs = lax.map(one_expert, (lookup, expert_gate_weight, expert_up_weight, expert_down_weight))
    flat_outputs = outputs.reshape(-1, width)
    flat_index = flat_slot.reshape(total_rows, TOPK)
    combined = jnp.zeros((total_rows, width), jnp.float32)
    for ranked in range(TOPK):
        combined = combined + flat_outputs[flat_index[:, ranked]].astype(jnp.float32) * chosen_expert_weight[:, ranked:ranked + 1]
    return combined.astype(jnp.bfloat16)

def reference(query_preactivation, forget_preactivation, value_input_rows, output_gate_preactivation, forget_floor_gap, extra_log_forget, head_output_gain, mixer_output_weight, second_batch_tokens, feedforward_norm_gain, chosen_expert_index, chosen_expert_weight, expert_gate_weight, expert_up_weight, expert_down_weight):
    mixer_output_first = mixer_portion(query_preactivation, forget_preactivation, value_input_rows, output_gate_preactivation, forget_floor_gap, extra_log_forget, head_output_gain, mixer_output_weight)
    moe_out = expert_part(second_batch_tokens, feedforward_norm_gain, chosen_expert_index, chosen_expert_weight, expert_gate_weight, expert_up_weight, expert_down_weight)
    return (mixer_output_first, moe_out)
```

```python
import functools

import jax
import jax.numpy as jnp
from jax import lax
from jax.experimental import pallas as pl
from jax.experimental.pallas import tpu as pltpu
from jax.sharding import PartitionSpec as P

KEY_DIM = 128
VAL_DIM = 64
BLOCK_POSITIONS = 64
TOPK = 2


epsilon = 1e-06


CHUNK = 256
NT = (((1,), (1,)), ((), ()))
TN = (((0,), (0,)), ((), ()))


def local_kernel(heads, q_ref, f_ref, v_ref, gap_ref, extra_ref, rec_ref, qdec_ref, carry_ref, state, base):
    step = pl.program_id(0)

    @pl.when(step == 0)
    def _():
        state[...] = jnp.zeros_like(state)
        base[...] = jnp.zeros_like(base)

    rows, vals = v_ref.shape
    q = q_ref[...].astype(jnp.float32)
    q = q / (1.0 + jnp.exp(-q))
    key = gap_ref[...] / (1.0 + jnp.exp(f_ref[...].astype(jnp.float32)))
    extra = extra_ref[...]
    log_forget = jnp.log(1.0 - key) + jnp.concatenate(
        [jnp.broadcast_to(extra[:, h : h + 1], (rows, KEY_DIM)) for h in range(heads)], axis=1
    )
    at = lax.broadcasted_iota(jnp.int32, (rows, rows), 0)
    of = lax.broadcasted_iota(jnp.int32, (rows, rows), 1)
    lower = jnp.where((at >= of) & (at // BLOCK_POSITIONS == of // BLOCK_POSITIONS), 1.0, 0.0)
    lower = lower.astype(jnp.bfloat16)
    high = log_forget.astype(jnp.bfloat16)
    low = (log_forget - high.astype(jnp.float32)).astype(jnp.bfloat16)
    cumulative = jnp.dot(lower, high, preferred_element_type=jnp.float32) + jnp.dot(
        lower, low, preferred_element_type=jnp.float32
    )
    causal = lax.broadcasted_iota(
        jnp.int32, (BLOCK_POSITIONS, BLOCK_POSITIONS), 0
    ) >= lax.broadcasted_iota(jnp.int32, (BLOCK_POSITIONS, BLOCK_POSITIONS), 1)
    lane_head = lax.broadcasted_iota(jnp.int32, (BLOCK_POSITIONS, vals), 1) // VAL_DIM
    held = [state[h] for h in range(heads)]
    before = base[...]
    half = BLOCK_POSITIONS // 2
    for b in range(rows // BLOCK_POSITIONS):
        part = slice(b * BLOCK_POSITIONS, (b + 1) * BLOCK_POSITIONS)
        cum = cumulative[part]
        mid, last = cum[half - 1 : half], cum[BLOCK_POSITIONS - 1 :]
        q_part = q[part]
        q_mid = (q_part * jnp.exp(cum - mid)).astype(jnp.bfloat16)
        k_mid = (key[part] * jnp.exp(mid - cum)).astype(jnp.bfloat16)
        qdec_ref[part, :] = (q_part * jnp.exp(cum + before)).astype(jnp.bfloat16)
        decay_mid, decay_last, decay_rest = jnp.exp(mid), jnp.exp(last), jnp.exp(last - mid)
        before = before + last
        values = v_ref[part, :]
        out = jnp.zeros((BLOCK_POSITIONS, vals), jnp.float32)
        for h in range(heads):
            lanes = slice(h * KEY_DIM, (h + 1) * KEY_DIM)
            across = lax.dot_general(
                q_mid[:, lanes],
                (held[h] * decay_mid[:, lanes]).astype(jnp.bfloat16),
                NT,
                preferred_element_type=jnp.float32,
            )
            scores = lax.dot_general(
                q_mid[:, lanes], k_mid[:, lanes], NT, preferred_element_type=jnp.float32
            )
            scores = jnp.where(causal, scores, 0.0).astype(jnp.bfloat16)
            within = jnp.dot(scores, values, preferred_element_type=jnp.float32)
            out = jnp.where(lane_head == h, within + across, out)
            update = lax.dot_general(
                values, k_mid[:, lanes], TN, preferred_element_type=jnp.float32
            )
            held[h] = held[h] * decay_last[:, lanes] + update * decay_rest[:, lanes]
        rec_ref[part, :] = out
    for h in range(heads):
        state[h] = held[h]
    base[...] = before

    @pl.when(step == pl.num_programs(0) - 1)
    def _():
        own = [held[h][h * VAL_DIM : (h + 1) * VAL_DIM] for h in range(heads)]
        carry_ref[:VAL_DIM, :] = jnp.concatenate(own, axis=1).astype(jnp.bfloat16)
        total = jnp.exp(before)
        carry_ref[VAL_DIM:, :] = jnp.broadcast_to(total, (16, total.shape[1])).astype(jnp.bfloat16)


def local_recurrence(query, forget, values, gap, extra):
    length, keys = query.shape
    heads, vals = keys // KEY_DIM, values.shape[1]

    def chunk(width):
        return pl.BlockSpec((CHUNK, width), lambda i: (i, 0))

    return pl.pallas_call(
        functools.partial(local_kernel, heads),
        grid=(length // CHUNK,),
        in_specs=[
            chunk(keys),
            chunk(keys),
            chunk(vals),
            pl.BlockSpec((1, keys), lambda i: (0, 0)),
            chunk(heads),
        ],
        out_specs=[
            chunk(vals),
            chunk(keys),
            pl.BlockSpec((VAL_DIM + 16, keys), lambda i: (0, 0)),
        ],
        out_shape=[
            jax.ShapeDtypeStruct((length, vals), jnp.float32),
            jax.ShapeDtypeStruct((length, keys), jnp.bfloat16),
            jax.ShapeDtypeStruct((VAL_DIM + 16, keys), jnp.bfloat16),
        ],
        scratch_shapes=[
            pltpu.VMEM((heads, vals, KEY_DIM), jnp.float32),
            pltpu.VMEM((1, keys), jnp.float32),
        ],
        cost_estimate=pl.CostEstimate(
            flops=10_000_000_000, bytes_accessed=6_000_000, transcendentals=3_000_000
        ),
        name="local_recurrence",
    )(query, forget, values, gap.reshape(1, keys), extra)


def gate_kernel(heads, places, place_ref, rec_ref, qdec_ref, carry_ref, gain_ref, gate_ref, out_ref, held):
    rows, vals = rec_ref.shape

    @pl.when(pl.program_id(0) == 0)
    def _():
        place = place_ref[0]
        total = jnp.zeros((VAL_DIM, heads * KEY_DIM), jnp.float32)
        for i in range(places):
            decay = carry_ref[i, VAL_DIM:, :].astype(jnp.float32)[:1]
            joined = total * decay + carry_ref[i, :VAL_DIM, :].astype(jnp.float32)
            total = jnp.where(i < place, joined, total)
        lane_head = lax.broadcasted_iota(jnp.int32, total.shape, 1) // KEY_DIM
        for h in range(heads):
            held[h * VAL_DIM : (h + 1) * VAL_DIM, :] = jnp.where(lane_head == h, total, 0.0).astype(
                jnp.bfloat16
            )

    rec = rec_ref[...] + lax.dot_general(
        qdec_ref[...], held[...], NT, preferred_element_type=jnp.float32
    )
    at = lax.broadcasted_iota(jnp.int32, (vals, vals), 0) // VAL_DIM
    of = lax.broadcasted_iota(jnp.int32, (vals, vals), 1) // VAL_DIM
    average = jnp.where(at == of, 1.0 / VAL_DIM, 0.0).astype(jnp.bfloat16)
    square = rec * rec
    high = square.astype(jnp.bfloat16)
    low = (square - high.astype(jnp.float32)).astype(jnp.bfloat16)
    mean = jnp.dot(high, average, preferred_element_type=jnp.float32) + jnp.dot(
        low, average, preferred_element_type=jnp.float32
    )
    gate = gate_ref[...].astype(jnp.float32)
    gate = gate / (1.0 + jnp.exp(-gate))
    out_ref[...] = (rec * lax.rsqrt(mean + epsilon) * gain_ref[...] * gate).astype(jnp.bfloat16)


def gated_output(rec, qdec, carries, gain, gate):
    length, vals = rec.shape
    keys = qdec.shape[1]
    heads = keys // KEY_DIM
    rows = 2 * CHUNK

    def chunk(width):
        return pl.BlockSpec((rows, width), lambda i: (i, 0))

    return pl.pallas_call(
        functools.partial(gate_kernel, heads, carries.shape[0]),
        grid=(length // rows,),
        in_specs=[
            pl.BlockSpec(memory_space=pltpu.SMEM),
            chunk(vals),
            chunk(keys),
            pl.BlockSpec(carries.shape, lambda i: (0, 0, 0)),
            pl.BlockSpec((1, vals), lambda i: (0, 0)),
            chunk(vals),
        ],
        out_specs=chunk(vals),
        out_shape=jax.ShapeDtypeStruct((length, vals), jnp.bfloat16),
        scratch_shapes=[pltpu.VMEM((vals, keys), jnp.bfloat16)],
        cost_estimate=pl.CostEstimate(
            flops=2_000_000_000, bytes_accessed=3_000_000, transcendentals=1_000_000
        ),
        name="gated_output",
    )(lax.axis_index("ep").reshape(1), rec, qdec, carries, gain.reshape(1, vals), gate)


def norm_rows(tokens, row_gain):
    tokens_float = tokens.astype(jnp.float32)
    factor = lax.rsqrt(jnp.mean(tokens_float * tokens_float, axis=-1, keepdims=True) + epsilon)
    return (tokens_float * factor * row_gain).astype(jnp.bfloat16)


def slot_positions(blocks, experts_all):
    flattened = blocks.reshape(blocks.shape[0], -1)
    onehot = (flattened[..., None] == jnp.arange(experts_all, dtype=jnp.int32)).astype(jnp.int32)
    earlier = jnp.cumsum(onehot, axis=1) - onehot
    return jnp.sum(earlier * onehot, axis=-1).reshape(blocks.shape)


def fill_slots(rows_in, blocks, slot_ids, experts_all, capacity):
    groups = blocks.shape[0]
    sub_rows = blocks.shape[1]
    group_ids = jnp.arange(groups, dtype=jnp.int32)[:, None, None]
    target = (group_ids * experts_all + blocks) * capacity + slot_ids
    sources = jnp.broadcast_to(
        jnp.arange(sub_rows, dtype=jnp.int32)[None, :, None] + group_ids * sub_rows, blocks.shape
    )
    lookup = (
        jnp.full((groups * experts_all * capacity,), -1, jnp.int32)
        .at[target.reshape(-1)]
        .set(sources.reshape(-1))
    )
    gathered = rows_in.reshape(groups * sub_rows, -1)[jnp.maximum(lookup, 0)]
    filled = jnp.where((lookup >= 0)[:, None], gathered, jnp.zeros((), gathered.dtype))
    return filled.reshape(groups, experts_all, capacity, -1)


def on_device(
    query_preactivation,
    forget_preactivation,
    value_input_rows,
    output_gate_preactivation,
    forget_floor_gap,
    extra_log_forget,
    head_output_gain,
    mixer_output_weight,
    second_batch_tokens,
    feedforward_norm_gain,
    chosen_expert_index,
    chosen_expert_weight,
    expert_gate_weight,
    expert_up_weight,
    expert_down_weight,
):
    local_experts = expert_gate_weight.shape[0]
    places = lax.axis_size("ep")
    experts_all = local_experts * places
    groups = lax.axis_size("tp")
    width = second_batch_tokens.shape[1]
    sub_rows = second_batch_tokens.shape[0] // groups
    capacity = max(2, sub_rows * TOPK * 5 // (4 * experts_all))
    place = lax.axis_index("ep")
    position = lax.axis_index("tp")
    pairs = groups // 2
    side = lax.rem(position, 2)

    all_routes = chosen_expert_index.reshape(pairs, 2, sub_rows, TOPK)
    routes = lax.dynamic_index_in_dim(all_routes, side, 1, False)
    all_tokens = second_batch_tokens.reshape(pairs, 2, sub_rows, width)
    tokens = lax.dynamic_index_in_dim(all_tokens, side, 1, False)
    slots = slot_positions(routes, experts_all)
    outgoing = fill_slots(
        norm_rows(tokens, feedforward_norm_gain), routes, slots, experts_all, capacity
    )
    outgoing, query_preactivation = lax.optimization_barrier((outgoing, query_preactivation))
    outgoing = outgoing.reshape(pairs, places, local_experts, capacity, width)
    arrived = []
    for step in range(places):
        block = lax.dynamic_index_in_dim(outgoing, place ^ step, 1, False)
        if step:
            block = lax.ppermute(block, "ep", [(i, i ^ step) for i in range(places)])
        arrived.append(block)
    partners = [(i, i ^ 1) for i in range(groups)]
    shape = (pairs, places, local_experts, capacity, width)
    others = [lax.ppermute(block, "tp", partners) for block in arrived]
    own_side = jnp.stack(arrived, axis=1)
    other_side = jnp.stack(others, axis=1)

    recurrent, query_decayed, carry = local_recurrence(
        query_preactivation,
        forget_preactivation,
        value_input_rows,
        forget_floor_gap,
        extra_log_forget,
    )
    carries = lax.all_gather(carry, "ep")
    mixed = gated_output(
        recurrent, query_decayed, carries, head_output_gain, output_gate_preactivation
    )
    mixed_all = lax.all_gather(mixed, "tp", axis=1, tiled=True)

    def experts(rows):
        gate_part = jnp.einsum(
            "tsecd,edf->tsecf", rows, expert_gate_weight, preferred_element_type=jnp.float32
        )
        up_part = jnp.einsum(
            "tsecd,edf->tsecf", rows, expert_up_weight, preferred_element_type=jnp.float32
        )
        hidden = (jax.nn.silu(gate_part) * up_part).astype(jnp.bfloat16)
        product = jnp.einsum(
            "tsecf,efd->tsecd", hidden, expert_down_weight, preferred_element_type=jnp.float32
        )
        return product.astype(jnp.bfloat16)

    other_side, mixed = lax.optimization_barrier((other_side, mixed))
    for_partner = experts(other_side)
    own_side, for_partner = lax.optimization_barrier((own_side, for_partner))
    from_partner = lax.ppermute(for_partner, "tp", partners)
    product = experts(own_side).astype(jnp.float32) + from_partner.astype(jnp.float32)
    product, mixed_all = lax.optimization_barrier((product.astype(jnp.bfloat16), mixed_all))
    to_return = lax.psum_scatter(
        product,
        "tp",
        scatter_dimension=0,
        tiled=True,
        axis_index_groups=[list(range(c, groups, 2)) for c in range(2)],
    )
    to_return = to_return.reshape(shape[1:])
    mixer_output_first = jnp.dot(
        mixed_all, mixer_output_weight, preferred_element_type=jnp.float32
    ).astype(jnp.bfloat16)
    returned = []
    for step in range(places):
        block = to_return[step]
        if step:
            block = lax.ppermute(block, "ep", [(i, i ^ step) for i in range(places)])
        returned.append(block)
    results = jnp.concatenate(returned, axis=0).reshape(experts_all * capacity, width)
    own_routes = lax.dynamic_index_in_dim(routes, position // 2, 0, False)
    own_slots = lax.dynamic_index_in_dim(slots, position // 2, 0, False)
    own_weights = lax.dynamic_slice_in_dim(chosen_expert_weight, position * sub_rows, sub_rows, 0)
    holder = (own_routes // local_experts) ^ place
    flat_index = (holder * local_experts + own_routes % local_experts) * capacity + own_slots
    combined = jnp.zeros((sub_rows, width), jnp.float32)
    for ranked in range(TOPK):
        combined = (
            combined
            + results[flat_index[:, ranked]].astype(jnp.float32)
            * own_weights[:, ranked : ranked + 1]
        )
    return (mixer_output_first, combined.astype(jnp.bfloat16))


def solution(mesh):
    placed = (
        P("ep", "tp"),
        P("ep", "tp"),
        P("ep", "tp"),
        P("ep", "tp"),
        P("tp"),
        P("ep", "tp"),
        P("tp"),
        P(None, "tp"),
        P("ep", None),
        P(),
        P("ep", None),
        P("ep", None),
        P("ep", None, "tp"),
        P("ep", None, "tp"),
        P("ep", "tp", None),
    )
    return jax.shard_map(
        on_device,
        mesh=mesh,
        in_specs=placed,
        out_specs=(P("ep", "tp"), P(("ep", "tp"), None)),
        check_vma=False,
    )
```
